32 devices in a mesh: grp: 2 (over x), fs: 4 (over y, core), tp: 4 (over z).
Axes of the slice: x: 2, y: 2, z: 4, core: 2. Of those that a mesh axis runs over, the one named last changes fastest.
Arguments:
- stream: bfloat16 [4096, 2048], P(('grp', 'fs', 'tp')), parts along dimension 0, may hold values from -4 to 4
- gain_first: bfloat16 [2048], replicated, may hold values from 0.099609375 to 1.8984375
- gate_first: bfloat16 [2048, 4096], P('fs', 'tp'), may hold values from -0.125 to 0.125
- up_first: bfloat16 [2048, 4096], P('fs', 'tp'), may hold values from -0.125 to 0.125
- down_first: bfloat16 [4096, 2048], P('tp', 'fs'), may hold values from -0.09375 to 0.09375
- gain_second: bfloat16 [2048], replicated, may hold values from 0.099609375 to 1.8984375
- gate_second: bfloat16 [2048, 4096], P('fs', 'tp'), may hold values from -0.125 to 0.125
- up_second: bfloat16 [2048, 4096], P('fs', 'tp'), may hold values from -0.125 to 0.125
- down_second: bfloat16 [4096, 2048], P('tp', 'fs'), may hold values from -0.09375 to 0.09375
Outputs:
- result: bfloat16 [4096, 2048], P(('grp', 'fs', 'tp')), parts along dimension 0
The draws below stay inside these ranges and needn't reach their ends.
There are 2 independent parts, one for each index of `grp`. The reference program is written for one: setup_inputs(seed, part) draws one part's arguments, and reference() takes and returns one part's arrays. A program takes and returns all parts, laid end to end along the dimension named above; an argument that names none is the same for every part. Nothing has to cross between parts.
All inputs are finite; a program needn't handle non-finite values.
Results may differ from the reference program's by a relative error of at most 0.018.
Values may be sent and summed in bfloat16 or wider, within the bound.
A program may use at most 64 MiB of HBM per device.

```python
import jax
import jax.numpy as jnp
from jax import lax

D = 2048
FF = 4096
TOKENS = 2048
N_TP = 4


def block_scale(rng, extent, shards, smallest, largest):
    level = 1.0
    for position, blocks in shards:
        steps = jax.random.uniform(jax.random.fold_in(jax.random.fold_in(rng, 6), position), (blocks,), jnp.float32, smallest / len(shards), largest / len(shards))
        level = level * jnp.repeat(jnp.exp(steps), extent[position] // blocks).reshape((-1,) + (1,) * (len(extent) - 1 - position))
    return level


def scatter_about(stream_key, dims, deviation, bound, cuts=(), kind=jnp.bfloat16):
    drawn = deviation * jax.random.normal(stream_key, dims, jnp.float32)
    if cuts:
        drawn = drawn * block_scale(stream_key, dims, cuts, -0.22, 0.18)
    return jnp.clip(drawn, -bound, bound).astype(kind)


def setup_inputs(seed: int = 0, part: int = 0) -> dict:
    streams_of = jax.random.split(jax.random.key(seed), 10)
    part_keys = jax.random.split(jax.random.fold_in(streams_of[9], part), 10)
    return {
        "stream": scatter_about(part_keys[0], (TOKENS, D), 0.5, 4.0, ((0, 16),)),
        "gain_first": jnp.clip(1.0 + 0.18 * jax.random.normal(streams_of[1], (D,), jnp.float32), 0.099609375, 1.8984375).astype(jnp.bfloat16),
        "gate_first": scatter_about(streams_of[2], (D, FF), D ** -0.5, 0.125, ((0, 4), (1, 4))),
        "up_first": scatter_about(streams_of[3], (D, FF), D ** -0.5, 0.125, ((0, 4), (1, 4))),
        "down_first": scatter_about(streams_of[4], (FF, D), FF ** -0.5, 0.09375, ((0, 4), (1, 4))),
        "gain_second": jnp.clip(1.0 + 0.18 * jax.random.normal(streams_of[5], (D,), jnp.float32), 0.099609375, 1.8984375).astype(jnp.bfloat16),
        "gate_second": scatter_about(streams_of[6], (D, FF), D ** -0.5, 0.125, ((0, 4), (1, 4))),
        "up_second": scatter_about(streams_of[7], (D, FF), D ** -0.5, 0.125, ((0, 4), (1, 4))),
        "down_second": scatter_about(streams_of[8], (FF, D), FF ** -0.5, 0.09375, ((0, 4), (1, 4))),
    }


def half_branch(stream, gain, w_gate, w_up, w_down):
    stream_f = stream.astype(jnp.float32)
    normed = (stream_f * lax.rsqrt(lax.optimization_barrier(jnp.mean(stream_f * stream_f, axis=-1, keepdims=True)) + 1e-06) * gain.astype(jnp.float32)).astype(jnp.bfloat16)
    gate_act = jnp.dot(normed, w_gate, preferred_element_type=jnp.float32)
    up_act = jnp.dot(normed, w_up, preferred_element_type=jnp.float32)
    hidden = (jax.nn.silu(gate_act) * up_act).astype(jnp.bfloat16)
    span_width = FF // N_TP
    summed = jnp.zeros(stream.shape, jnp.float32)
    for shard in range(N_TP):
        partial_sum = jnp.dot(hidden[:, shard * span_width:(shard + 1) * span_width], w_down[shard * span_width:(shard + 1) * span_width], preferred_element_type=jnp.float32).astype(jnp.bfloat16)
        partial_sum = lax.optimization_barrier(partial_sum)
        summed = summed + partial_sum.astype(jnp.float32)
    return (stream_f + 0.5 * summed).astype(jnp.bfloat16)

def reference(stream, gain_first, gate_first, up_first, down_first, gain_second, gate_second, up_second, down_second):
    middle = half_branch(stream, gain_first, gate_first, up_first, down_first)
    return half_branch(middle, gain_second, gate_second, up_second, down_second)
```

```python
import functools

import jax
import jax.numpy as jnp
from jax import lax
from jax.experimental import pallas as pl
from jax.experimental.pallas import tpu as pltpu
from jax.sharding import PartitionSpec as P

MESH = pl.DeviceIdType.MESH
CORES = 2
PIECES = 4
BATCHES = 4
SLOT = 1.2
LAG = 3.2
HOP = 3.0
VMEM_LIMIT = 60 * 1024 * 1024


def kernel(
    sizes,
    stream, gain_a, gain_b, gate_a, up_a, down_a, gate_b, up_b, down_b,
    out,
    gu, dn, xg, hid, part, rbuf, acc, mid,
    y_s, y_r, x_s, x_r, c_s, c_r, f_s, f_r, l_s, ag_s, ag_r, rs_s, rs_r,
):
    G, m, n, T, D, F, J, K = sizes
    Y = m // CORES
    C = D // J
    R = T // K
    U = 6 * PIECES
    weights = (gate_a, up_a, down_a, gate_b, up_b, down_b)
    gains = (gain_a, gain_b)
    g = lax.axis_index("grp")
    fs = lax.axis_index("fs")
    me = lax.axis_index("tp")
    y = fs // CORES
    c = lax.rem(fs, CORES)
    mate = y * CORES + (CORES - 1 - c)
    right = lax.rem(me + 1, n)
    left = lax.rem(me + n - 1, n)

    def row_of(k):
        return lax.rem(y + k + Y, Y) * CORES + c

    def grp_of(i):
        return lax.rem(g + i + G, G)

    barrier = pltpu.get_barrier_semaphore()
    for k in range(1, Y):
        pl.semaphore_signal(barrier, inc=1, device_id={"fs": row_of(k)}, device_id_type=MESH)
    for i in range(1, G):
        pl.semaphore_signal(barrier, inc=1, device_id={"grp": grp_of(i)}, device_id_type=MESH)
    pl.semaphore_signal(barrier, inc=1, device_id={"fs": mate}, device_id_type=MESH)

    @pl.when(me < n - 1)
    def _():
        pl.semaphore_signal(barrier, inc=1, device_id={"tp": right}, device_id_type=MESH)

    @pl.when(me > 0)
    def _():
        pl.semaphore_signal(barrier, inc=1, device_id={"tp": left}, device_id_type=MESH)

    @pl.when(jnp.logical_and(me > 0, me < n - 1))
    def _():
        pl.semaphore_wait(barrier, Y - 1 + G - 1 + 1 + 2)

    @pl.when(jnp.logical_not(jnp.logical_and(me > 0, me < n - 1)))
    def _():
        pl.semaphore_wait(barrier, Y - 1 + G - 1 + 1 + 1)

    def rows_of(a):
        return weights[a].shape[0]

    def piece_rows(u, h):
        rows = rows_of(u // PIECES) // G
        sub = rows // PIECES
        return pl.multiple_of(h * rows + (u % PIECES) * sub, sub), sub

    def own(u, h):
        off, sub = piece_rows(u, h)
        return weights[u // PIECES].at[pl.ds(off, sub), :]

    def place(a, j, off, count):
        b, t = a // 3, a % 3
        if t < 2:
            return gu.at[b, t, pl.ds(pl.multiple_of(j * rows_of(a) + off, count), count), :]
        cols = D // m
        return dn.at[b, pl.ds(off, count), pl.ds(pl.multiple_of(j * cols, cols), cols)]

    def slot(u, j, h):
        off, sub = piece_rows(u, h)
        return place(u // PIECES, j, off, sub)

    def whole(a, j):
        return place(a, j, 0, rows_of(a))

    def remote(src, dst, ss, rs, dev):
        return pltpu.make_async_remote_copy(
            src_ref=src, dst_ref=dst, send_sem=ss, recv_sem=rs, device_id=dev, device_id_type=MESH
        )

    def local_copy(a):
        return pltpu.make_async_copy(weights[a], whole(a, fs), l_s.at[a])

    def y_copy(a, k):
        return remote(own(a, g), slot(a, fs, g), y_s.at[a, k - 1], y_r.at[a, k - 1], {"fs": row_of(k)})

    def y_arrived(a, k):
        remote(own(a, g), slot(a, row_of(-k), g), y_s.at[a, k - 1], y_r.at[a, k - 1], {"fs": row_of(k)}).wait_recv()

    def c_copy(a):
        return remote(weights[a], whole(a, fs), c_s.at[a], c_r.at[a], {"fs": mate})

    def c_arrived(a):
        remote(weights[a], whole(a, mate), c_s.at[a], c_r.at[a], {"fs": mate}).wait_recv()

    def x_copy(a, k, i):
        where = slot(a, row_of(-k), g)
        return remote(where, where, x_s.at[a, k - 1, i - 1], x_r.at[a, k - 1, i - 1], {"grp": grp_of(i)})

    def x_arrived(a, k, i):
        where = slot(a, row_of(-k), grp_of(-i))
        remote(where, where, x_s.at[a, k - 1, i - 1], x_r.at[a, k - 1, i - 1], {"grp": grp_of(i)}).wait_recv()

    def f_copy(a, k, i):
        where = slot(a, row_of(-k), grp_of(-i))
        return remote(where, where, f_s.at[a, k - 1, i], f_r.at[a, k - 1, i], {"fs": mate})

    def f_arrived(a, k, i):
        row = lax.rem(y - k + Y, Y) * CORES + (CORES - 1 - c)
        where = slot(a, row, grp_of(-i))
        remote(where, where, f_s.at[a, k - 1, i], f_r.at[a, k - 1, i], {"fs": mate}).wait_recv()

    def y_event(a):
        for k in range(1, Y):
            y_arrived(a, k)
            for i in range(1, G):
                x_copy(a, k, i).start()
            f_copy(a, k, 0).start()

    def x_event(a):
        for k in range(1, Y):
            for i in range(1, G):
                x_arrived(a, k, i)
                f_copy(a, k, i).start()

    def nearby(a):
        local_copy(a).wait()
        c_arrived(a)

    def complete(a):
        for u in range(a * PIECES, (a + 1) * PIECES):
            for k in range(1, Y):
                for i in range(G):
                    f_arrived(u, k, i)

    def rows_at(blk):
        return pl.ds(pl.multiple_of(blk * R, R), R)

    def cols_at(j):
        return pl.ds(pl.multiple_of(lax.rem(y + j, J) * C, C), C)

    def ag(b, way, k, blk):
        where = xg.at[b, k, rows_at(blk), :]
        return remote(where, where, ag_s.at[b, way, k, blk], ag_r.at[b, k, blk], {"tp": right if way == 0 else left})

    def ag_step(b, k, s):
        for way in range(2):
            blk = me - s if way == 0 else me + s

            @pl.when(blk >= 0 if way == 0 else blk < n)
            def _():
                ag(b, way, k, blk).wait_recv()

                @pl.when(me < n - 1 if way == 0 else me > 0)
                def _():
                    ag(b, way, k, blk).start()

    def normalize(b, k, source):
        rows = pl.ds(k * R, R)
        v = source[rows, :].astype(jnp.float32)
        scale = lax.rsqrt(jnp.mean(v * v, axis=-1, keepdims=True) + 1e-06)
        xg[b, k, rows_at(me), :] = (v * scale * gains[b][...].astype(jnp.float32)).astype(jnp.bfloat16)

        @pl.when(me < n - 1)
        def _():
            ag(b, 0, k, me).start()

        @pl.when(me > 0)
        def _():
            ag(b, 1, k, me).start()

    def hidden_of(b, k):
        tile = min(512, F)

        @pl.loop(0, F // tile)
        def _(q):
            cols = pl.ds(pl.multiple_of(q * tile, tile), tile)
            x = xg[b, k]
            gate = jnp.dot(x, gu[b, 0, :, cols], preferred_element_type=jnp.float32)
            up = jnp.dot(x, gu[b, 1, :, cols], preferred_element_type=jnp.float32)
            hid[k, :, cols] = (gate / (1.0 + jnp.exp(-gate)) * up).astype(jnp.bfloat16)

    def rs(b, way, k, j, d):
        return remote(
            part.at[b, k, j, rows_at(d), :], rbuf.at[b, way, k, j, rows_at(d), :],
            rs_s.at[b, k, j, d], rs_r.at[b, way, k, j, d], {"tp": right if way == 0 else left},
        )

    def partial_of(b, k, j):
        tile = min(512, C)

        @pl.loop(0, C // tile)
        def _(q):
            cols = pl.ds(pl.multiple_of(lax.rem(y + j, J) * C + q * tile, tile), tile)
            dst = pl.ds(pl.multiple_of(q * tile, tile), tile)
            part[b, k, j, :, dst] = jnp.dot(
                hid[k], dn[b, :, cols], preferred_element_type=jnp.float32
            ).astype(jnp.bfloat16)

        @pl.when(me == 0)
        def _():
            for d in range(n - 1, 0, -1):
                rs(b, 0, k, j, d).start()

        @pl.when(me == n - 1)
        def _():
            for d in range(n - 1):
                rs(b, 1, k, j, d).start()

    def relay_one(b, way, k, j, d):
        rs(b, way, k, j, d).wait_recv()
        part[b, k, j, rows_at(d), :] = (
            part[b, k, j, rows_at(d), :].astype(jnp.float32)
            + rbuf[b, way, k, j, rows_at(d), :].astype(jnp.float32)
        ).astype(jnp.bfloat16)
        rs(b, way, k, j, d).start()

    def relay(b, k, j, q):
        @pl.when(me == q)
        def _():
            @pl.loop(0, n - 1 - q)
            def _(i):
                relay_one(b, 0, k, j, n - 1 - i)

        @pl.when(n - 1 - me == q)
        def _():
            @pl.loop(0, n - 1 - q)
            def _(i):
                relay_one(b, 1, k, j, i)

    def finish(b, k, j, source, target):
        rows = pl.ds(k * R, R)
        acc[...] = part[b, k, j, rows_at(me), :].astype(jnp.float32)

        @pl.when(me > 0)
        def _():
            rs(b, 0, k, j, me).wait_recv()
            acc[...] += rbuf[b, 0, k, j, rows_at(me), :].astype(jnp.float32)

        @pl.when(me < n - 1)
        def _():
            rs(b, 1, k, j, me).wait_recv()
            acc[...] += rbuf[b, 1, k, j, rows_at(me), :].astype(jnp.float32)

        target[rows, cols_at(j)] = (
            source[rows, cols_at(j)].astype(jnp.float32) + 0.5 * acc[...]
        ).astype(jnp.bfloat16)

    for u in range(U):
        for k in range(1, Y):
            y_copy(u, k).start()
    for k in range(K):
        normalize(0, k, stream)
    for a in range(6):
        local_copy(a).start()
        c_copy(a).start()

    for kind, args in plan(n, J, K):
        with jax.named_scope(kind + "_" + "_".join(map(str, args))):
            if kind == "y":
                y_event(*args)
            elif kind == "x":
                x_event(*args)
            elif kind == "c":
                complete(*args)
            elif kind == "o":
                nearby(*args)
            elif kind == "a":
                ag_step(*args)
            elif kind == "h":
                hidden_of(*args)
            elif kind == "p":
                partial_of(*args)
            elif kind == "r":
                relay(*args)
            elif kind == "f":
                finish(*args, *((stream, mid) if args[0] == 0 else (mid, out)))
            elif kind == "n":
                normalize(*args, mid)

    for a in range(6):
        c_copy(a).wait_send()
    for u in range(U):
        for k in range(1, Y):
            y_copy(u, k).wait_send()
            f_copy(u, k, 0).wait_send()
            for i in range(1, G):
                x_copy(u, k, i).wait_send()
                f_copy(u, k, i).wait_send()

    @pl.loop(0, 2)
    def _(b):
        @pl.loop(0, K)
        def _(k):
            @pl.loop(0, n)
            def _(d):
                @pl.when(jnp.logical_and(d <= me, me < n - 1))
                def _():
                    ag(b, 0, k, d).wait_send()

                @pl.when(jnp.logical_and(d >= me, me > 0))
                def _():
                    ag(b, 1, k, d).wait_send()

                @pl.loop(0, J)
                def _(j):
                    @pl.when(d > me)
                    def _():
                        rs(b, 0, k, j, d).wait_send()

                    @pl.when(d < me)
                    def _():
                        rs(b, 1, k, j, d).wait_send()


def plan(n, J, K):
    items = []

    def at(time, kind, *args):
        items.append((time, len(items), kind, args))

    U = 6 * PIECES
    whole = J * K
    tau = whole / PIECES
    for u in range(U):
        at(tau * (u + 1) + 0.3, "y", u)
        at(tau * (u + 2) + 0.7, "x", u)
    for s in range(1, n):
        for k in range(K):
            at(whole * (s - 1) + J * (k + 1) + 0.5, "a", 0, k, s)
    ready = [tau * ((a + 1) * PIECES + 1) + 0.8 for a in range(6)]
    for a in range(6):
        at(ready[a], "c", a)
        at(0.2 + whole * a / 8, "o", a)
    slot = (n - 1) * SLOT
    order = []
    for k in range(0, K, 2):
        pair = range(k, min(k + 2, K))
        order += [(q, j) for j in range(J) for q in pair] if k == 0 else [(q, j) for q in pair for j in range(J)]
    start = ready[1] + 0.1
    arrived = [whole * (n - 2) + J * (k + 1) + 0.6 for k in range(K)]
    for b in range(2):
        begun = set()
        done = [0] * K
        now = start
        for k, j in order:
            now = max(now, arrived[k], ready[3 * b + 2] if j > 0 else 0)
            if k not in begun:
                begun.add(k)
                at(now + 0.01, "h", b, k)
            at(now + 0.02, "p", b, k, j)
            for q in range(1, n - 1):
                at(now + LAG * q, "r", b, k, j, q)
            at(now + LAG * (n - 1), "f", b, k, j)
            done[k] = max(done[k], now + LAG * (n - 1))
            now += slot
        if b == 0:
            for k in range(K):
                at(done[k] + 0.03, "n", 1, k)
                for s in range(1, n):
                    at(done[k] + 0.04 + HOP * s, "a", 1, k, s)
                arrived[k] = done[k] + 0.05 + HOP * (n - 1)
            start = max(now, ready[4] + 0.1)
    items.sort(key=lambda item: item[:2])
    return [item[2:] for item in items]


def local(sizes_of_mesh, stream, gain_a, gate_a, up_a, down_a, gain_b, gate_b, up_b, down_b):
    G, m, n = sizes_of_mesh
    T, D = stream.shape
    F = gate_a.shape[1]
    Y = m // CORES
    J = Y if Y <= 2 else 1
    K = BATCHES
    U = 6 * PIECES
    bf16 = jnp.bfloat16
    vmem = pl.BlockSpec(memory_space=pltpu.VMEM)
    anywhere = pl.BlockSpec(memory_space=pl.ANY)
    dma = pltpu.SemaphoreType.DMA
    return pl.pallas_call(
        functools.partial(kernel, (G, m, n, T, D, F, J, K)),
        out_shape=jax.ShapeDtypeStruct((T, D), bf16),
        in_specs=[vmem] * 3 + [anywhere] * 6,
        out_specs=vmem,
        scratch_shapes=[
            pltpu.VMEM((2, 2, D, F), bf16),
            pltpu.VMEM((2, F, D), bf16),
            pltpu.VMEM((2, K, n * T // K, D), bf16),
            pltpu.VMEM((K, n * T // K, F), bf16),
            pltpu.VMEM((2, K, J, n * T // K, D // J), bf16),
            pltpu.VMEM((2, 2, K, J, n * T // K, D // J), bf16),
            pltpu.VMEM((T // K, D // J), jnp.float32),
            pltpu.VMEM((T, D), bf16),
            dma((U, Y - 1)), dma((U, Y - 1)),
            dma((U, Y - 1, G - 1)), dma((U, Y - 1, G - 1)),
            dma((6,)), dma((6,)),
            dma((U, Y - 1, G)), dma((U, Y - 1, G)),
            dma((6,)),
            dma((2, 2, K, n)), dma((2, K, n)),
            dma((2, K, J, n)), dma((2, 2, K, J, n)),
        ],
        compiler_params=pltpu.CompilerParams(
            collective_id=0, has_side_effects=True, vmem_limit_bytes=VMEM_LIMIT
        ),
    )(
        stream, gain_a.reshape(1, D), gain_b.reshape(1, D),
        gate_a, up_a, down_a, gate_b, up_b, down_b,
    )


def solution(mesh):
    shape = mesh.shape
    in_specs = (
        P(("grp", "fs", "tp"), None),
        P(),
        P("fs", "tp"),
        P("fs", "tp"),
        P("tp", "fs"),
        P(),
        P("fs", "tp"),
        P("fs", "tp"),
        P("tp", "fs"),
    )
    out_specs = P(("grp", "fs", "tp"), None)
    body = functools.partial(local, (shape["grp"], shape["fs"], shape["tp"]))
    return jax.shard_map(body, mesh=mesh, in_specs=in_specs, out_specs=out_specs, check_vma=False)
```

```python
import functools

import jax
import jax.numpy as jnp
from jax import lax
from jax.experimental import pallas as pl
from jax.experimental.pallas import tpu as pltpu
from jax.sharding import PartitionSpec as P

MESH = pl.DeviceIdType.MESH
CORES = 2
PIECES = (8, 8, 8, 4, 4, 4)
UNITS = [(a, p) for a in range(6) for p in range(PIECES[a])]
BATCHES = 4
TUNE = (0.0, (3.35, 4.32), (3.02, 5.12), (7.18, 13.38), (2.82, 6.01), 4.7, 2.0, 2.9)
VMEM_LIMIT = 60 * 1024 * 1024


def kernel(
    sizes,
    stream_hbm, gain_a, gain_b, gate_a, up_a, down_a, gate_b, up_b, down_b,
    out_hbm,
    gu, dn, xg, hid, part, rbuf, acc, mid, stream, out, scale_a, scale_b,
    i_s, o_s, y_s, y_r, x_s, x_r, c_s, c_r, f_s, f_r, l_s, ag_s, ag_r, rs_s, rs_r,
):
    G, m, n, T, D, F, J, K = sizes
    Y = m // CORES
    C = D // J
    R = T // K
    U = len(UNITS)
    gains = (scale_a, scale_b)
    weights = (gate_a, up_a, down_a, gate_b, up_b, down_b)
    g = lax.axis_index("grp")
    fs = lax.axis_index("fs")
    me = lax.axis_index("tp")
    y = fs // CORES
    c = lax.rem(fs, CORES)
    mate = y * CORES + (CORES - 1 - c)
    right = lax.rem(me + 1, n)
    left = lax.rem(me + n - 1, n)

    def row_of(k):
        return lax.rem(y + k + Y, Y) * CORES + c

    def grp_of(i):
        return lax.rem(g + i + G, G)

    def load(k):
        rows = pl.ds(k * R, R)
        return pltpu.make_async_copy(stream_hbm.at[rows, :], stream.at[rows, :], i_s.at[k])

    def save(k):
        rows = pl.ds(k * R, R)
        return pltpu.make_async_copy(out.at[rows, :], out_hbm.at[rows, :], o_s.at[k])

    def gain_load(b):
        return pltpu.make_async_copy((gain_a, gain_b)[b], gains[b], i_s.at[K + b])

    barrier = pltpu.get_barrier_semaphore()
    for k in range(1, Y):
        pl.semaphore_signal(barrier, inc=1, device_id={"fs": row_of(k)}, device_id_type=MESH)
    for i in range(1, G):
        pl.semaphore_signal(barrier, inc=1, device_id={"grp": grp_of(i)}, device_id_type=MESH)
    pl.semaphore_signal(barrier, inc=1, device_id={"fs": mate}, device_id_type=MESH)

    @pl.when(me < n - 1)
    def _():
        pl.semaphore_signal(barrier, inc=1, device_id={"tp": right}, device_id_type=MESH)

    @pl.when(me > 0)
    def _():
        pl.semaphore_signal(barrier, inc=1, device_id={"tp": left}, device_id_type=MESH)

    for k in range(K):
        load(k).start()
    for b in range(2):
        gain_load(b).start()

    @pl.when(jnp.logical_and(me > 0, me < n - 1))
    def _():
        pl.semaphore_wait(barrier, Y - 1 + G - 1 + 1 + 2)

    @pl.when(jnp.logical_not(jnp.logical_and(me > 0, me < n - 1)))
    def _():
        pl.semaphore_wait(barrier, Y - 1 + G - 1 + 1 + 1)

    def rows_of(a):
        return weights[a].shape[0]

    def piece_rows(u, h):
        a, p = UNITS[u]
        rows = rows_of(a) // G
        sub = rows // PIECES[a]
        return pl.multiple_of(h * rows + p * sub, sub), sub

    def own(u, h):
        off, sub = piece_rows(u, h)
        return weights[UNITS[u][0]].at[pl.ds(off, sub), :]

    def place(a, j, off, count):
        b, t = a // 3, a % 3
        if t < 2:
            return gu.at[b, t, pl.ds(pl.multiple_of(j * rows_of(a) + off, count), count), :]
        cols = D // m
        return dn.at[b, pl.ds(off, count), pl.ds(pl.multiple_of(j * cols, cols), cols)]

    def slot(u, j, h):
        off, sub = piece_rows(u, h)
        return place(UNITS[u][0], j, off, sub)

    def whole(a, j):
        return place(a, j, 0, rows_of(a))

    def remote(src, dst, ss, rs, dev):
        return pltpu.make_async_remote_copy(
            src_ref=src, dst_ref=dst, send_sem=ss, recv_sem=rs, device_id=dev, device_id_type=MESH
        )

    def local_copy(a):
        return pltpu.make_async_copy(weights[a], whole(a, fs), l_s.at[a])

    def y_copy(a, k):
        return remote(own(a, g), slot(a, fs, g), y_s, y_r.at[a, k - 1], {"fs": row_of(k)})

    def y_arrived(a, k):
        remote(own(a, g), slot(a, row_of(-k), g), y_s, y_r.at[a, k - 1], {"fs": row_of(k)}).wait_recv()

    def c_copy(a):
        return remote(weights[a], whole(a, fs), c_s, c_r.at[a], {"fs": mate})

    def c_arrived(a):
        remote(weights[a], whole(a, mate), c_s, c_r.at[a], {"fs": mate}).wait_recv()

    def x_copy(a, k, i):
        where = slot(a, row_of(-k), g)
        return remote(where, where, x_s, x_r.at[a, k - 1, i - 1], {"grp": grp_of(i)})

    def x_arrived(a, k, i):
        where = slot(a, row_of(-k), grp_of(-i))
        remote(where, where, x_s, x_r.at[a, k - 1, i - 1], {"grp": grp_of(i)}).wait_recv()

    def f_copy(a, k, i):
        where = slot(a, row_of(-k), grp_of(-i))
        return remote(where, where, f_s, f_r.at[UNITS[a][0]], {"fs": mate})

    def y_event(a):
        for k in range(1, Y):
            y_arrived(a, k)
            for i in range(1, G):
                x_copy(a, k, i).start()
            f_copy(a, k, 0).start()

    def x_event(a):
        for k in range(1, Y):
            for i in range(1, G):
                x_arrived(a, k, i)
                f_copy(a, k, i).start()

    def nearby(a):
        local_copy(a).wait()
        c_arrived(a)

    far = (Y - 1) * (D // m)

    def complete(a):
        where = gu.at[0, 0, pl.ds(0, far), :]
        remote(where, where, f_s, f_r.at[a], {"fs": mate}).wait_recv()

    def sent():
        for rows, sem in (
            (D // m, c_s), (far // G, y_s), (far // G * (G - 1), x_s), (far, f_s),
        ):
            where = gu.at[:, :, pl.ds(0, 6 * rows // 4), :]
            remote(where, where, sem, f_r.at[0], {"fs": mate}).wait_send()

    def rows_at(blk):
        return pl.ds(pl.multiple_of(blk * R, R), R)

    def cols_at(j):
        return pl.ds(pl.multiple_of(lax.rem(y + j, J) * C, C), C)

    def ag(b, way, k, blk):
        where = xg.at[b, k, rows_at(blk), :]
        return remote(where, where, ag_s.at[b, way], ag_r.at[k, blk], {"tp": right if way == 0 else left})

    def ag_step(b, k, s):
        for way in range(2):
            blk = me - s if way == 0 else me + s

            @pl.when(blk >= 0 if way == 0 else blk < n)
            def _():
                ag(b, way, k, blk).wait_recv()

                @pl.when(me < n - 1 if way == 0 else me > 0)
                def _():
                    ag(b, way, k, blk).start()

    def normalize(b, k, source):
        rows = pl.ds(k * R, R)
        v = source[rows, :].astype(jnp.float32)
        scale = lax.rsqrt(jnp.mean(v * v, axis=-1, keepdims=True) + 1e-06)
        xg[b, k, rows_at(me), :] = (v * scale * gains[b][...].astype(jnp.float32).reshape(1, D)).astype(jnp.bfloat16)

        @pl.when(me < n - 1)
        def _():
            ag(b, 0, k, me).start()

        @pl.when(me > 0)
        def _():
            ag(b, 1, k, me).start()

    def hidden_of(b, k):
        tile = min(512, F)

        @pl.loop(0, F // tile)
        def _(q):
            cols = pl.ds(pl.multiple_of(q * tile, tile), tile)
            x = xg[b, k]
            gate = jnp.dot(x, gu[b, 0, :, cols], preferred_element_type=jnp.float32)
            up = jnp.dot(x, gu[b, 1, :, cols], preferred_element_type=jnp.float32)
            hid[k, :, cols] = (gate / (1.0 + jnp.exp(-gate)) * up).astype(jnp.bfloat16)

    def rs(b, way, k, j, d, last=False):
        arrived = rs_r.at[k, j, n if last and way == 1 else d]
        return remote(
            part.at[b, k, j, rows_at(d), :], rbuf.at[b, way, k, j, rows_at(d), :],
            rs_s.at[b], arrived, {"tp": right if way == 0 else left},
        )

    def partial_of(b, k, j):
        tile = min(512, C)

        @pl.loop(0, C // tile)
        def _(q):
            cols = pl.ds(pl.multiple_of(lax.rem(y + j, J) * C + q * tile, tile), tile)
            dst = pl.ds(pl.multiple_of(q * tile, tile), tile)
            part[b, k, j, :, dst] = jnp.dot(
                hid[k], dn[b, :, cols], preferred_element_type=jnp.float32
            ).astype(jnp.bfloat16)

    def hop(b, k, j, q, e):
        for way in range(2):
            @pl.when(me == (q if way == 0 else n - 1 - q))
            def _():
                d = q + e if way == 0 else n - 1 - q - e
                if q > 0:
                    rs(b, way, k, j, d).wait_recv()
                    part[b, k, j, rows_at(d), :] = (
                        part[b, k, j, rows_at(d), :].astype(jnp.float32)
                        + rbuf[b, way, k, j, rows_at(d), :].astype(jnp.float32)
                    ).astype(jnp.bfloat16)
                rs(b, way, k, j, d, e == 1).start()

    def finish(b, k, j, source, target):
        rows = pl.ds(k * R, R)
        acc[...] = part[b, k, j, rows_at(me), :].astype(jnp.float32)

        @pl.when(me > 0)
        def _():
            rs(b, 0, k, j, me, True).wait_recv()
            acc[...] += rbuf[b, 0, k, j, rows_at(me), :].astype(jnp.float32)

        @pl.when(me < n - 1)
        def _():
            rs(b, 1, k, j, me, True).wait_recv()
            acc[...] += rbuf[b, 1, k, j, rows_at(me), :].astype(jnp.float32)

        target[rows, cols_at(j)] = (
            source[rows, cols_at(j)].astype(jnp.float32) + 0.5 * acc[...]
        ).astype(jnp.bfloat16)

    def gathered(b):
        for way in range(2):
            for i in range(1, n):
                @pl.when(me == (i - 1 if way == 0 else n - i))
                def _():
                    where = xg.at[b, :, pl.ds(0, i * R), :]
                    remote(where, where, ag_s.at[b, way], ag_s.at[b, way], {"fs": mate}).wait_send()

    def ship_done(b):
        where = part.at[b, :, :, pl.ds(0, (n - 1) * R), :]
        remote(where, where, rs_s.at[b], rs_s.at[b], {"fs": mate}).wait_send()

    for u in range(PIECES[0]):
        for k in range(1, Y):
            y_copy(u, k).start()
    for b in range(2):
        gain_load(b).wait()
    for k in range(K):
        load(k).wait()
        normalize(0, k, stream)
    for u in range(PIECES[0], U):
        for k in range(1, Y):
            y_copy(u, k).start()

    for kind, args in plan(n, J, K):
        with jax.named_scope(kind + "_" + "_".join(map(str, args))):
            if kind == "y":
                y_event(*args)
            elif kind == "x":
                x_event(*args)
            elif kind == "c":
                complete(*args)
            elif kind == "o":
                nearby(*args)
            elif kind == "a":
                ag_step(*args)
            elif kind == "h":
                hidden_of(*args)
            elif kind == "p":
                partial_of(*args)
            elif kind == "r":
                hop(*args)
            elif kind == "f":
                finish(*args, *((stream, mid) if args[0] == 0 else (mid, out)))
            elif kind == "n":
                normalize(*args, mid)
            elif kind == "s":
                save(*args).start()
            elif kind == "d":
                sent()
            elif kind == "g":
                gathered(*args)
            elif kind == "t":
                ship_done(*args)
            elif kind == "l":
                local_copy(*args).start()
                c_copy(*args).start()

    ship_done(1)
    for k in range(K):
        save(k).wait()


def plan(n, J, K, tune=TUNE):
    items = []

    def at(time, kind, *args):
        items.append((time, len(items), kind, args))

    b0, slots, lag, ends, hops, late, own, early = tune
    whole = J * K
    ready = []
    came = 0
    for u, (a, p) in enumerate(UNITS):
        tau = whole / PIECES[a]
        came += tau
        delay = early if a < 2 else late
        at(came + 0.8, "y", u)
        at(came + tau + delay, "x", u)
        if p == PIECES[a] - 1:
            ready.append(came + tau + delay + 0.1)
    for s in range(1, n):
        for k in range(K):
            at(whole * (s - 1) + J * (k + 1) + 0.9, "a", 0, k, s)
    for a in range(6):
        at(ready[a + 1 if a % 3 == 0 else a], "c", a)
        at(a * own, "l", a)
        at(ready[1] if a < 3 else ready[4], "o", a)
    arrived = [whole * (n - 2) + J * (k + 1) + 1.0 for k in range(K)]
    for b in range(2):
        first = min(3, K) if b == 0 else min(2, K)
        order = [(k, 0) for k in range(first)] + [(k, j) for k in range(first) for j in range(1, J)]
        order += [(k, j) for k in range(first, K) for j in range(J)]
        begun = set()
        done = [0] * K
        now = ready[1] + b0 if b == 0 else max(now, ready[4])
        for place, (k, j) in enumerate(order):
            now = max(now, arrived[k], ready[3 * b + 2] if j > 0 else 0)
            if k not in begun:
                begun.add(k)
                at(now + 0.01, "h", b, k)
            at(now + 0.02, "p", b, k, j)
            spread = b == 1 and k == K - 1
            for q in range(n - 1):
                for e in range(1, n - q):
                    wide = (n - 1 - q - e) / (n - 1)
                    if spread:
                        wide = wide * J + 0.03
                    at(now + 0.03 + lag[b] * q + wide * slots[b], "r", b, k, j, q, e)
            end = now + ends[b] + (0.01 * j if not spread else J * 0.5)
            at(end, "f", b, k, j)
            done[k] = max(done[k], end)
            now += slots[b]
        for k in range(K):
            if b == 0:
                at(done[k] + 0.03, "n", 1, k)
                for s in range(1, n):
                    at(done[k] + 0.04 + hops[k // ((K + 1) // 2)] * s, "a", 1, k, s)
                arrived[k] = done[k] + 0.05 + hops[k // ((K + 1) // 2)] * (n - 1)
            else:
                at(done[k] + 0.03, "s", k)
    at(now - slots[1], "d")
    for b in range(2):
        at(now - slots[1] * (2 - b), "g", b)
    at(now - slots[1], "t", 0)
    items.sort(key=lambda item: item[:2])
    return [item[2:] for item in items]


def local(sizes_of_mesh, stream, gain_a, gate_a, up_a, down_a, gain_b, gate_b, up_b, down_b):
    G, m, n = sizes_of_mesh
    T, D = stream.shape
    F = gate_a.shape[1]
    Y = m // CORES
    J = Y if Y <= 2 else 1
    K = BATCHES
    U = len(UNITS)
    bf16 = jnp.bfloat16
    anywhere = pl.BlockSpec(memory_space=pl.ANY)
    dma = pltpu.SemaphoreType.DMA
    return pl.pallas_call(
        functools.partial(kernel, (G, m, n, T, D, F, J, K)),
        out_shape=jax.ShapeDtypeStruct((T, D), bf16),
        in_specs=[anywhere] * 9,
        out_specs=anywhere,
        scratch_shapes=[
            pltpu.VMEM((2, 2, D, F), bf16),
            pltpu.VMEM((2, F, D), bf16),
            pltpu.VMEM((2, K, n * T // K, D), bf16),
            pltpu.VMEM((K, n * T // K, F), bf16),
            pltpu.VMEM((2, K, J, n * T // K, D // J), bf16),
            pltpu.VMEM((2, 2, K, J, n * T // K, D // J), bf16),
            pltpu.VMEM((T // K, D // J), jnp.float32),
            pltpu.VMEM((T, D), bf16),
            pltpu.VMEM((T, D), bf16),
            pltpu.VMEM((T, D), bf16),
            pltpu.VMEM((D,), bf16),
            pltpu.VMEM((D,), bf16),
            dma((K + 2,)), dma((K,)),
            dma(()), dma((U, Y - 1)),
            dma(()), dma((U, Y - 1, G - 1)),
            dma(()), dma((6,)),
            dma(()), dma((6,)),
            dma((6,)),
            dma((2, 2)), dma((K, n)),
            dma((2,)), dma((K, J, n + 1)),
        ],
        compiler_params=pltpu.CompilerParams(
            collective_id=0, has_side_effects=True, vmem_limit_bytes=VMEM_LIMIT
        ),
    )(
        stream, gain_a, gain_b,
        gate_a, up_a, down_a, gate_b, up_b, down_b,
    )


def solution(mesh):
    shape = mesh.shape
    in_specs = (
        P(("grp", "fs", "tp"), None),
        P(),
        P("fs", "tp"),
        P("fs", "tp"),
        P("tp", "fs"),
        P(),
        P("fs", "tp"),
        P("fs", "tp"),
        P("tp", "fs"),
    )
    out_specs = P(("grp", "fs", "tp"), None)
    body = functools.partial(local, (shape["grp"], shape["fs"], shape["tp"]))
    return jax.shard_map(body, mesh=mesh, in_specs=in_specs, out_specs=out_specs, check_vma=False)
```

```python
import functools

import jax
import jax.numpy as jnp
from jax import lax
from jax.experimental import pallas as pl
from jax.experimental.pallas import tpu as pltpu
from jax.sharding import PartitionSpec as P

MESH = pl.DeviceIdType.MESH
CORES = 2
PIECES = (8, 8, 8, 4, 4, 4)
UNITS = [(a, p) for a in range(6) for p in range(PIECES[a])]
BATCHES = 4
ORDER = (
    0, 2, 4, 72, 6, 8, 73, 74, 10, 12, 85, 14, 16, 18, 20, 22, 1, 76, 24, 26,
    78, 15, 7, 88, 75, 91, 5, 3, 89, 17, 77, 11, 28, 30, 34, 29, 82, 9, 36, 25,
    31, 23, 32, 27, 21, 19, 13, 84, 92, 87, 80, 86, 102, 38, 103, 105, 106, 81, 40, 111,
    112, 44, 115, 42, 94, 120, 46, 114, 121, 104, 124, 79, 39, 123, 113, 48, 83, 108, 117, 116,
    45, 97, 43, 126, 33, 47, 107, 35, 37, 41, 50, 90, 129, 132, 52, 131, 130, 137, 118, 140,
    49, 109, 134, 145, 139, 127, 133, 54, 125, 119, 153, 110, 122, 135, 148, 162, 56, 142, 136, 170,
    128, 141, 51, 58, 53, 138, 154, 143, 150, 171, 157, 165, 147, 60, 100, 144, 62, 174, 55, 93,
    98, 146, 151, 149, 59, 156, 164, 155, 66, 172, 167, 159, 95, 68, 175, 152, 101, 57, 178, 168,
    63, 61, 173, 96, 158, 64, 186, 70, 160, 187, 176, 163, 189, 166, 190, 65, 261, 188, 161, 67,
    179, 169, 182, 71, 69, 99, 204, 206, 177, 195, 207, 191, 196, 258, 205, 212, 199, 180, 197, 215,
    183, 192, 214, 198, 181, 220, 221, 229, 209, 208, 184, 232, 217, 223, 185, 201, 193, 210, 224, 237,
    194, 200, 231, 238, 241, 246, 234, 202, 249, 213, 211, 226, 218, 260, 248, 216, 240, 203, 243, 251,
    235, 233, 230, 244, 219, 225, 239, 222, 227, 247, 242, 250, 252, 236, 245, 228, 254, 256, 255, 253,
    259, 257,
)
TUNE = (0.0, (3.35, 4.32), (3.02, 5.12), (7.18, 13.38), (2.82, 6.01), 4.7, 2.0, 2.9)
VMEM_LIMIT = 60 * 1024 * 1024


def kernel(
    sizes,
    stream_hbm, gain_a, gain_b, gate_a, up_a, down_a, gate_b, up_b, down_b,
    out_hbm,
    gu, dn, xg, hid, part, rbuf, acc, mid, stream, out, scale_a, scale_b,
    i_s, o_s, y_s, y_r, x_s, x_r, c_s, c_r, f_s, f_r, l_s, ag_s, ag_r, rs_s, rs_r,
):
    G, m, n, T, D, F, J, K = sizes
    Y = m // CORES
    C = D // J
    R = T // K
    U = len(UNITS)
    gains = (scale_a, scale_b)
    weights = (gate_a, up_a, down_a, gate_b, up_b, down_b)
    g = lax.axis_index("grp")
    fs = lax.axis_index("fs")
    me = lax.axis_index("tp")
    y = fs // CORES
    c = lax.rem(fs, CORES)
    mate = y * CORES + (CORES - 1 - c)
    right = lax.rem(me + 1, n)
    left = lax.rem(me + n - 1, n)

    def row_of(k):
        return lax.rem(y + k + Y, Y) * CORES + c

    def grp_of(i):
        return lax.rem(g + i + G, G)

    def load(k):
        rows = pl.ds(k * R, R)
        return pltpu.make_async_copy(stream_hbm.at[rows, :], stream.at[rows, :], i_s.at[k])

    def save(k):
        rows = pl.ds(k * R, R)
        return pltpu.make_async_copy(out.at[rows, :], out_hbm.at[rows, :], o_s.at[k])

    def gain_load(b):
        return pltpu.make_async_copy((gain_a, gain_b)[b], gains[b], i_s.at[K + b])

    barrier = pltpu.get_barrier_semaphore()
    for k in range(1, Y):
        pl.semaphore_signal(barrier, inc=1, device_id={"fs": row_of(k)}, device_id_type=MESH)
    for i in range(1, G):
        pl.semaphore_signal(barrier, inc=1, device_id={"grp": grp_of(i)}, device_id_type=MESH)
    pl.semaphore_signal(barrier, inc=1, device_id={"fs": mate}, device_id_type=MESH)

    @pl.when(me < n - 1)
    def _():
        pl.semaphore_signal(barrier, inc=1, device_id={"tp": right}, device_id_type=MESH)

    @pl.when(me > 0)
    def _():
        pl.semaphore_signal(barrier, inc=1, device_id={"tp": left}, device_id_type=MESH)

    for k in range(K):
        load(k).start()
    for b in range(2):
        gain_load(b).start()

    @pl.when(jnp.logical_and(me > 0, me < n - 1))
    def _():
        pl.semaphore_wait(barrier, Y - 1 + G - 1 + 1 + 2)

    @pl.when(jnp.logical_not(jnp.logical_and(me > 0, me < n - 1)))
    def _():
        pl.semaphore_wait(barrier, Y - 1 + G - 1 + 1 + 1)

    def rows_of(a):
        return weights[a].shape[0]

    def piece_rows(u, h):
        a, p = UNITS[u]
        rows = rows_of(a) // G
        sub = rows // PIECES[a]
        return pl.multiple_of(h * rows + p * sub, sub), sub

    def own(u, h):
        off, sub = piece_rows(u, h)
        return weights[UNITS[u][0]].at[pl.ds(off, sub), :]

    def place(a, j, off, count):
        b, t = a // 3, a % 3
        if t < 2:
            return gu.at[b, t, pl.ds(pl.multiple_of(j * rows_of(a) + off, count), count), :]
        cols = D // m
        return dn.at[b, pl.ds(off, count), pl.ds(pl.multiple_of(j * cols, cols), cols)]

    def slot(u, j, h):
        off, sub = piece_rows(u, h)
        return place(UNITS[u][0], j, off, sub)

    def whole(a, j):
        return place(a, j, 0, rows_of(a))

    def remote(src, dst, ss, rs, dev):
        return pltpu.make_async_remote_copy(
            src_ref=src, dst_ref=dst, send_sem=ss, recv_sem=rs, device_id=dev, device_id_type=MESH
        )

    def local_copy(a):
        return pltpu.make_async_copy(weights[a], whole(a, fs), l_s.at[a])

    def y_copy(a, k):
        return remote(own(a, g), slot(a, fs, g), y_s, y_r.at[a, k - 1], {"fs": row_of(k)})

    def y_arrived(a, k):
        remote(own(a, g), slot(a, row_of(-k), g), y_s, y_r.at[a, k - 1], {"fs": row_of(k)}).wait_recv()

    def c_copy(a):
        return remote(weights[a], whole(a, fs), c_s, c_r.at[a], {"fs": mate})

    def c_arrived(a):
        remote(weights[a], whole(a, mate), c_s, c_r.at[a], {"fs": mate}).wait_recv()

    def x_copy(a, k, i):
        where = slot(a, row_of(-k), g)
        return remote(where, where, x_s, x_r.at[a, k - 1, i - 1], {"grp": grp_of(i)})

    def x_arrived(a, k, i):
        where = slot(a, row_of(-k), grp_of(-i))
        remote(where, where, x_s, x_r.at[a, k - 1, i - 1], {"grp": grp_of(i)}).wait_recv()

    def f_copy(a, k, i):
        where = slot(a, row_of(-k), grp_of(-i))
        return remote(where, where, f_s, f_r.at[UNITS[a][0]], {"fs": mate})

    def y_event(a):
        for k in range(1, Y):
            y_arrived(a, k)
            for i in range(1, G):
                x_copy(a, k, i).start()
            f_copy(a, k, 0).start()

    def x_event(a):
        for k in range(1, Y):
            for i in range(1, G):
                x_arrived(a, k, i)
                f_copy(a, k, i).start()

    def nearby(a):
        local_copy(a).wait()
        c_arrived(a)

    far = (Y - 1) * (D // m)

    def complete(a):
        where = gu.at[0, 0, pl.ds(0, far), :]
        remote(where, where, f_s, f_r.at[a], {"fs": mate}).wait_recv()

    def sent():
        for rows, sem in (
            (D // m, c_s), (far // G, y_s), (far // G * (G - 1), x_s), (far, f_s),
        ):
            where = gu.at[:, :, pl.ds(0, 6 * rows // 4), :]
            remote(where, where, sem, f_r.at[0], {"fs": mate}).wait_send()

    def rows_at(blk):
        return pl.ds(pl.multiple_of(blk * R, R), R)

    def cols_at(j):
        return pl.ds(pl.multiple_of(lax.rem(y + j, J) * C, C), C)

    def ag(b, way, k, blk):
        where = xg.at[b, k, rows_at(blk), :]
        return remote(where, where, ag_s.at[b, way], ag_r.at[k, blk], {"tp": right if way == 0 else left})

    def ag_step(b, k, s):
        for way in range(2):
            blk = me - s if way == 0 else me + s

            @pl.when(blk >= 0 if way == 0 else blk < n)
            def _():
                ag(b, way, k, blk).wait_recv()

                @pl.when(me < n - 1 if way == 0 else me > 0)
                def _():
                    ag(b, way, k, blk).start()

    def normalize(b, k, source):
        rows = pl.ds(k * R, R)
        v = source[rows, :].astype(jnp.float32)
        scale = lax.rsqrt(jnp.mean(v * v, axis=-1, keepdims=True) + 1e-06)
        xg[b, k, rows_at(me), :] = (v * scale * gains[b][...].astype(jnp.float32).reshape(1, D)).astype(jnp.bfloat16)

        @pl.when(me < n - 1)
        def _():
            ag(b, 0, k, me).start()

        @pl.when(me > 0)
        def _():
            ag(b, 1, k, me).start()

    def hidden_of(b, k):
        tile = min(512, F)

        @pl.loop(0, F // tile)
        def _(q):
            cols = pl.ds(pl.multiple_of(q * tile, tile), tile)
            x = xg[b, k]
            gate = jnp.dot(x, gu[b, 0, :, cols], preferred_element_type=jnp.float32)
            up = jnp.dot(x, gu[b, 1, :, cols], preferred_element_type=jnp.float32)
            hid[k, :, cols] = (gate / (1.0 + jnp.exp(-gate)) * up).astype(jnp.bfloat16)

    def rs(b, way, k, j, d, last=False):
        arrived = rs_r.at[k, j, n if last and way == 1 else d]
        return remote(
            part.at[b, k, j, rows_at(d), :], rbuf.at[b, way, k, j, rows_at(d), :],
            rs_s.at[b], arrived, {"tp": right if way == 0 else left},
        )

    def partial_of(b, k, j):
        tile = min(512, C)

        @pl.loop(0, C // tile)
        def _(q):
            cols = pl.ds(pl.multiple_of(lax.rem(y + j, J) * C + q * tile, tile), tile)
            dst = pl.ds(pl.multiple_of(q * tile, tile), tile)
            part[b, k, j, :, dst] = jnp.dot(
                hid[k], dn[b, :, cols], preferred_element_type=jnp.float32
            ).astype(jnp.bfloat16)

    def hop(b, k, j, q, e):
        for way in range(2):
            @pl.when(me == (q if way == 0 else n - 1 - q))
            def _():
                d = q + e if way == 0 else n - 1 - q - e
                if q > 0:
                    rs(b, way, k, j, d).wait_recv()
                    part[b, k, j, rows_at(d), :] = (
                        part[b, k, j, rows_at(d), :].astype(jnp.float32)
                        + rbuf[b, way, k, j, rows_at(d), :].astype(jnp.float32)
                    ).astype(jnp.bfloat16)
                rs(b, way, k, j, d, e == 1).start()

    def finish(b, k, j, source, target):
        rows = pl.ds(k * R, R)
        acc[...] = part[b, k, j, rows_at(me), :].astype(jnp.float32)

        @pl.when(me > 0)
        def _():
            rs(b, 0, k, j, me, True).wait_recv()
            acc[...] += rbuf[b, 0, k, j, rows_at(me), :].astype(jnp.float32)

        @pl.when(me < n - 1)
        def _():
            rs(b, 1, k, j, me, True).wait_recv()
            acc[...] += rbuf[b, 1, k, j, rows_at(me), :].astype(jnp.float32)

        target[rows, cols_at(j)] = (
            source[rows, cols_at(j)].astype(jnp.float32) + 0.5 * acc[...]
        ).astype(jnp.bfloat16)

    def gathered(b):
        for way in range(2):
            for i in range(1, n):
                @pl.when(me == (i - 1 if way == 0 else n - i))
                def _():
                    where = xg.at[b, :, pl.ds(0, i * R), :]
                    remote(where, where, ag_s.at[b, way], ag_s.at[b, way], {"fs": mate}).wait_send()

    def ship_done(b):
        where = part.at[b, :, :, pl.ds(0, (n - 1) * R), :]
        remote(where, where, rs_s.at[b], rs_s.at[b], {"fs": mate}).wait_send()

    for u in range(PIECES[0]):
        for k in range(1, Y):
            y_copy(u, k).start()
    for b in range(2):
        gain_load(b).wait()
    for k in range(K):
        load(k).wait()
        normalize(0, k, stream)
    for u in range(PIECES[0], U):
        for k in range(1, Y):
            y_copy(u, k).start()

    for kind, args in plan(n, J, K):
        with jax.named_scope(kind + "_" + "_".join(map(str, args))):
            if kind == "y":
                y_event(*args)
            elif kind == "x":
                x_event(*args)
            elif kind == "c":
                complete(*args)
            elif kind == "o":
                nearby(*args)
            elif kind == "a":
                ag_step(*args)
            elif kind == "h":
                hidden_of(*args)
            elif kind == "p":
                partial_of(*args)
            elif kind == "r":
                hop(*args)
            elif kind == "f":
                finish(*args, *((stream, mid) if args[0] == 0 else (mid, out)))
            elif kind == "n":
                normalize(*args, mid)
            elif kind == "s":
                save(*args).start()
            elif kind == "d":
                sent()
            elif kind == "g":
                gathered(*args)
            elif kind == "t":
                ship_done(*args)
            elif kind == "l":
                local_copy(*args).start()
                c_copy(*args).start()

    ship_done(1)
    for k in range(K):
        save(k).wait()


def plan(n, J, K, tune=TUNE):
    items = []

    def at(time, kind, *args):
        items.append((time, len(items), kind, args))

    b0, slots, lag, ends, hops, late, own, early = tune
    whole = J * K
    ready = []
    came = 0
    for u, (a, p) in enumerate(UNITS):
        tau = whole / PIECES[a]
        came += tau
        delay = early if a < 2 else late
        at(came + 0.8, "y", u)
        at(came + tau + delay, "x", u)
        if p == PIECES[a] - 1:
            ready.append(came + tau + delay + 0.1)
    for s in range(1, n):
        for k in range(K):
            at(whole * (s - 1) + J * (k + 1) + 0.9, "a", 0, k, s)
    for a in range(6):
        at(ready[a + 1 if a % 3 == 0 else a], "c", a)
        at(a * own, "l", a)
        at(ready[1] if a < 3 else ready[4], "o", a)
    arrived = [whole * (n - 2) + J * (k + 1) + 1.0 for k in range(K)]
    for b in range(2):
        first = min(3, K) if b == 0 else min(2, K)
        order = [(k, 0) for k in range(first)] + [(k, j) for k in range(first) for j in range(1, J)]
        order += [(k, j) for k in range(first, K) for j in range(J)]
        begun = set()
        done = [0] * K
        now = ready[1] + b0 if b == 0 else max(now, ready[4])
        for place, (k, j) in enumerate(order):
            now = max(now, arrived[k], ready[3 * b + 2] if j > 0 else 0)
            if k not in begun:
                begun.add(k)
                at(now + 0.01, "h", b, k)
            at(now + 0.02, "p", b, k, j)
            spread = b == 1 and k == K - 1
            for q in range(n - 1):
                for e in range(1, n - q):
                    wide = (n - 1 - q - e) / (n - 1)
                    if spread:
                        wide = wide * J + 0.03
                    at(now + 0.03 + lag[b] * q + wide * slots[b], "r", b, k, j, q, e)
            end = now + ends[b] + (0.01 * j if not spread else J * 0.5)
            at(end, "f", b, k, j)
            done[k] = max(done[k], end)
            now += slots[b]
        for k in range(K):
            if b == 0:
                at(done[k] + 0.03, "n", 1, k)
                for s in range(1, n):
                    at(done[k] + 0.04 + hops[k // ((K + 1) // 2)] * s, "a", 1, k, s)
                arrived[k] = done[k] + 0.05 + hops[k // ((K + 1) // 2)] * (n - 1)
            else:
                at(done[k] + 0.03, "s", k)
    at(now - slots[1], "d")
    for b in range(2):
        at(now - slots[1] * (2 - b), "g", b)
    at(now - slots[1], "t", 0)
    if (n, J, K) == (4, 2, 4) and ORDER:
        return [items[i][2:] for i in ORDER]
    items.sort(key=lambda item: item[:2])
    return [item[2:] for item in items]


def local(sizes_of_mesh, stream, gain_a, gate_a, up_a, down_a, gain_b, gate_b, up_b, down_b):
    G, m, n = sizes_of_mesh
    T, D = stream.shape
    F = gate_a.shape[1]
    Y = m // CORES
    J = Y if Y <= 2 else 1
    K = BATCHES
    U = len(UNITS)
    bf16 = jnp.bfloat16
    anywhere = pl.BlockSpec(memory_space=pl.ANY)
    dma = pltpu.SemaphoreType.DMA
    return pl.pallas_call(
        functools.partial(kernel, (G, m, n, T, D, F, J, K)),
        out_shape=jax.ShapeDtypeStruct((T, D), bf16),
        in_specs=[anywhere] * 9,
        out_specs=anywhere,
        scratch_shapes=[
            pltpu.VMEM((2, 2, D, F), bf16),
            pltpu.VMEM((2, F, D), bf16),
            pltpu.VMEM((2, K, n * T // K, D), bf16),
            pltpu.VMEM((K, n * T // K, F), bf16),
            pltpu.VMEM((2, K, J, n * T // K, D // J), bf16),
            pltpu.VMEM((2, 2, K, J, n * T // K, D // J), bf16),
            pltpu.VMEM((T // K, D // J), jnp.float32),
            pltpu.VMEM((T, D), bf16),
            pltpu.VMEM((T, D), bf16),
            pltpu.VMEM((T, D), bf16),
            pltpu.VMEM((D,), bf16),
            pltpu.VMEM((D,), bf16),
            dma((K + 2,)), dma((K,)),
            dma(()), dma((U, Y - 1)),
            dma(()), dma((U, Y - 1, G - 1)),
            dma(()), dma((6,)),
            dma(()), dma((6,)),
            dma((6,)),
            dma((2, 2)), dma((K, n)),
            dma((2,)), dma((K, J, n + 1)),
        ],
        compiler_params=pltpu.CompilerParams(
            collective_id=0, has_side_effects=True, vmem_limit_bytes=VMEM_LIMIT
        ),
    )(
        stream, gain_a, gain_b,
        gate_a, up_a, down_a, gate_b, up_b, down_b,
    )


def solution(mesh):
    shape = mesh.shape
    in_specs = (
        P(("grp", "fs", "tp"), None),
        P(),
        P("fs", "tp"),
        P("fs", "tp"),
        P("tp", "fs"),
        P(),
        P("fs", "tp"),
        P("fs", "tp"),
        P("tp", "fs"),
    )
    out_specs = P(("grp", "fs", "tp"), None)
    body = functools.partial(local, (shape["grp"], shape["fs"], shape["tp"]))
    return jax.shard_map(body, mesh=mesh, in_specs=in_specs, out_specs=out_specs, check_vma=False)
```

```python
import functools

import jax
import jax.numpy as jnp
from jax import lax
from jax.experimental import pallas as pl
from jax.experimental.pallas import tpu as pltpu
from jax.sharding import PartitionSpec as P

MESH = pl.DeviceIdType.MESH
CORES = 2
PIECES = (8, 8, 8, 4, 4, 4)
UNITS = [(a, p) for a in range(6) for p in range(PIECES[a])]
DIRECT = (sum(PIECES[:2]) - 1,)
HELD = sum(PIECES[:2])
RESUME = HELD - 2
BATCHES = 4
ORDER_FOR = (4, 2, 4)
ORDER = (
    85, 0, 2, 88, 4, 72, 1, 6, 91, 3, 8, 73, 5, 10, 94, 7, 12, 74, 9, 14,
    97, 11, 16, 75, 13, 18, 100, 15, 20, 76, 17, 22, 19, 24, 77, 21, 26, 23, 28, 78,
    25, 30, 27, 79, 31, 86, 89, 92, 32, 29, 80, 84, 87, 102, 34, 95, 103, 106, 81, 36,
    111, 101, 112, 105, 104, 82, 38, 40, 120, 121, 42, 108, 115, 39, 44, 123, 124, 83, 46, 37,
    41, 107, 153, 113, 48, 117, 35, 33, 122, 109, 114, 154, 125, 126, 47, 43, 45, 90, 50, 129,
    132, 131, 110, 118, 137, 145, 162, 127, 98, 140, 134, 52, 133, 130, 54, 142, 116, 148, 146, 128,
    135, 139, 56, 136, 150, 170, 143, 119, 55, 141, 147, 138, 259, 53, 58, 60, 157, 151, 171, 149,
    165, 62, 51, 57, 144, 174, 172, 49, 159, 163, 152, 167, 64, 66, 178, 164, 175, 61, 63, 59,
    93, 68, 173, 96, 186, 156, 168, 187, 188, 190, 160, 70, 166, 158, 176, 155, 189, 69, 65, 179,
    169, 161, 182, 67, 71, 99, 204, 192, 177, 206, 207, 195, 212, 196, 191, 215, 198, 199, 214, 180,
    205, 213, 181, 197, 220, 183, 209, 261, 221, 201, 184, 224, 200, 193, 216, 223, 229, 185, 208, 232,
    202, 237, 194, 246, 210, 217, 249, 238, 241, 248, 226, 203, 240, 225, 231, 234, 211, 218, 251, 247,
    219, 243, 235, 239, 250, 252, 258, 230, 227, 242, 260, 222, 254, 244, 233, 253, 245, 236, 257, 255,
    228, 256,
)
TUNE = (0.0, (3.35, 4.32), (3.02, 5.12), (7.18, 13.38), (2.82, 6.01), 4.7, 2.0, 2.9)
VMEM_LIMIT = 60 * 1024 * 1024


def kernel(
    sizes,
    stream_hbm, gain_a, gain_b, gate_a, up_a, down_a, gate_b, up_b, down_b,
    out,
    gu, dn, xg, hid, part, rbuf, acc, mid, stream, scale_a, scale_b,
    i_s, y_s, y_r, x_s, x_r, c_s, c_r, f_s, f_r, l_s, ag_s, ag_r, rs_s, rs_r,
):
    G, m, n, T, D, F, J, K = sizes
    Y = m // CORES
    C = D // J
    R = T // K
    U = len(UNITS)
    gains = (scale_a, scale_b)
    weights = (gate_a, up_a, down_a, gate_b, up_b, down_b)
    g = lax.axis_index("grp")
    fs = lax.axis_index("fs")
    me = lax.axis_index("tp")
    y = fs // CORES
    c = lax.rem(fs, CORES)
    mate = y * CORES + (CORES - 1 - c)
    right = lax.rem(me + 1, n)
    left = lax.rem(me + n - 1, n)

    def row_of(k):
        return lax.rem(y + k + Y, Y) * CORES + c

    def grp_of(i):
        return lax.rem(g + i + G, G)

    def load(k):
        rows = pl.ds(k * R, R)
        return pltpu.make_async_copy(stream_hbm.at[rows, :], stream.at[rows, :], i_s.at[k])

    def gain_load(b):
        return pltpu.make_async_copy((gain_a, gain_b)[b], gains[b], i_s.at[K + b])

    barrier = pltpu.get_barrier_semaphore()
    for k in range(1, Y):
        pl.semaphore_signal(barrier, inc=1, device_id={"fs": row_of(k)}, device_id_type=MESH)
    for i in range(1, G):
        pl.semaphore_signal(barrier, inc=1, device_id={"grp": grp_of(i)}, device_id_type=MESH)
    pl.semaphore_signal(barrier, inc=1, device_id={"fs": mate}, device_id_type=MESH)

    @pl.when(me < n - 1)
    def _():
        pl.semaphore_signal(barrier, inc=1, device_id={"tp": right}, device_id_type=MESH)

    @pl.when(me > 0)
    def _():
        pl.semaphore_signal(barrier, inc=1, device_id={"tp": left}, device_id_type=MESH)

    for k in range(K):
        load(k).start()
    for b in range(2):
        gain_load(b).start()

    @pl.when(jnp.logical_and(me > 0, me < n - 1))
    def _():
        pl.semaphore_wait(barrier, Y - 1 + G - 1 + 1 + 2)

    @pl.when(jnp.logical_not(jnp.logical_and(me > 0, me < n - 1)))
    def _():
        pl.semaphore_wait(barrier, Y - 1 + G - 1 + 1 + 1)

    def rows_of(a):
        return weights[a].shape[0]

    def piece_rows(u, h):
        a, p = UNITS[u]
        rows = rows_of(a) // G
        sub = rows // PIECES[a]
        return pl.multiple_of(h * rows + p * sub, sub), sub

    def own(u, h):
        off, sub = piece_rows(u, h)
        return weights[UNITS[u][0]].at[pl.ds(off, sub), :]

    def place(a, j, off, count):
        b, t = a // 3, a % 3
        if t < 2:
            return gu.at[b, t, pl.ds(pl.multiple_of(j * rows_of(a) + off, count), count), :]
        cols = D // m
        return dn.at[b, pl.ds(off, count), pl.ds(pl.multiple_of(j * cols, cols), cols)]

    def slot(u, j, h):
        off, sub = piece_rows(u, h)
        return place(UNITS[u][0], j, off, sub)

    def whole(a, j):
        return place(a, j, 0, rows_of(a))

    def remote(src, dst, ss, rs, dev):
        return pltpu.make_async_remote_copy(
            src_ref=src, dst_ref=dst, send_sem=ss, recv_sem=rs, device_id=dev, device_id_type=MESH
        )

    def local_copy(a):
        return pltpu.make_async_copy(weights[a], whole(a, fs), l_s.at[a])

    def y_copy(a, k):
        return remote(own(a, g), slot(a, fs, g), y_s, y_r.at[a, k - 1], {"fs": row_of(k)})

    def y_arrived(a, k):
        remote(own(a, g), slot(a, row_of(-k), g), y_s, y_r.at[a, k - 1], {"fs": row_of(k)}).wait_recv()

    def c_copy(a):
        return remote(weights[a], whole(a, fs), c_s, c_r.at[a], {"fs": mate})

    def c_arrived(a):
        remote(weights[a], whole(a, mate), c_s, c_r.at[a], {"fs": mate}).wait_recv()

    def x_copy(a, k, i):
        where = slot(a, row_of(-k), g)
        return remote(where, where, x_s, x_r.at[a, k - 1, i - 1], {"grp": grp_of(i)})

    def x_arrived(a, k, i):
        where = slot(a, row_of(-k), grp_of(-i))
        remote(where, where, x_s, x_r.at[a, k - 1, i - 1], {"grp": grp_of(i)}).wait_recv()

    def f_copy(a, k, i):
        where = slot(a, row_of(-k), grp_of(-i))
        return remote(where, where, f_s, f_r.at[UNITS[a][0]], {"fs": mate})

    def y_send(a):
        for k in range(1, Y):
            y_copy(a, k).start()
            for i in range(1, G):
                if a in DIRECT:
                    h = grp_of(-i)
                    remote(
                        own(a, h), slot(a, fs, h), x_s, x_r.at[a, k - 1, i - 1], {"fs": row_of(k)}
                    ).start()

    def y_event(a):
        for k in range(1, Y):
            y_arrived(a, k)
            for i in range(1, G):
                if a not in DIRECT:
                    x_copy(a, k, i).start()
            f_copy(a, k, 0).start()

    def x_event(a):
        for k in range(1, Y):
            for i in range(1, G):
                x_arrived(a, k, i)
                f_copy(a, k, i).start()

    def nearby(a):
        local_copy(a).wait()
        c_arrived(a)

    far = (Y - 1) * (D // m)

    def complete(a):
        where = gu.at[0, 0, pl.ds(0, far), :]
        remote(where, where, f_s, f_r.at[a], {"fs": mate}).wait_recv()

    def sent():
        for rows, sem in (
            (D // m, c_s), (far // G, y_s), (far // G * (G - 1), x_s), (far, f_s),
        ):
            where = gu.at[:, :, pl.ds(0, 6 * rows // 4), :]
            remote(where, where, sem, f_r.at[0], {"fs": mate}).wait_send()

    def rows_at(blk):
        return pl.ds(pl.multiple_of(blk * R, R), R)

    def cols_at(j):
        return pl.ds(pl.multiple_of(lax.rem(y + j, J) * C, C), C)

    def ag(b, way, k, blk):
        where = xg.at[b, k, rows_at(blk), :]
        return remote(where, where, ag_s.at[b, way], ag_r.at[k, blk], {"tp": right if way == 0 else left})

    def ag_step(b, k, s):
        for way in range(2):
            blk = me - s if way == 0 else me + s

            @pl.when(blk >= 0 if way == 0 else blk < n)
            def _():
                ag(b, way, k, blk).wait_recv()

                @pl.when(me < n - 1 if way == 0 else me > 0)
                def _():
                    ag(b, way, k, blk).start()

    def normalize(b, k, source):
        rows = pl.ds(k * R, R)
        v = source[rows, :].astype(jnp.float32)
        scale = lax.rsqrt(jnp.mean(v * v, axis=-1, keepdims=True) + 1e-06)
        xg[b, k, rows_at(me), :] = (v * scale * gains[b][...].astype(jnp.float32).reshape(1, D)).astype(jnp.bfloat16)

        @pl.when(me < n - 1)
        def _():
            ag(b, 0, k, me).start()

        @pl.when(me > 0)
        def _():
            ag(b, 1, k, me).start()

    def hidden_of(b, k):
        tile = min(512, F)

        @pl.loop(0, F // tile)
        def _(q):
            cols = pl.ds(pl.multiple_of(q * tile, tile), tile)
            x = xg[b, k]
            gate = jnp.dot(x, gu[b, 0, :, cols], preferred_element_type=jnp.float32)
            up = jnp.dot(x, gu[b, 1, :, cols], preferred_element_type=jnp.float32)
            hid[k, :, cols] = (gate / (1.0 + jnp.exp(-gate)) * up).astype(jnp.bfloat16)

    def rs(b, way, k, j, d, last=False):
        arrived = rs_r.at[k, j, n if last and way == 1 else d]
        return remote(
            part.at[b, k, j, rows_at(d), :], rbuf.at[b, way, k, j, rows_at(d), :],
            rs_s.at[b], arrived, {"tp": right if way == 0 else left},
        )

    def partial_of(b, k, j):
        tile = min(512, C)

        @pl.loop(0, C // tile)
        def _(q):
            cols = pl.ds(pl.multiple_of(lax.rem(y + j, J) * C + q * tile, tile), tile)
            dst = pl.ds(pl.multiple_of(q * tile, tile), tile)
            part[b, k, j, :, dst] = jnp.dot(
                hid[k], dn[b, :, cols], preferred_element_type=jnp.float32
            ).astype(jnp.bfloat16)

    def hop(b, k, j, q, e):
        for way in range(2):
            @pl.when(me == (q if way == 0 else n - 1 - q))
            def _():
                d = q + e if way == 0 else n - 1 - q - e
                if q > 0:
                    rs(b, way, k, j, d).wait_recv()
                    part[b, k, j, rows_at(d), :] = (
                        part[b, k, j, rows_at(d), :].astype(jnp.float32)
                        + rbuf[b, way, k, j, rows_at(d), :].astype(jnp.float32)
                    ).astype(jnp.bfloat16)
                rs(b, way, k, j, d, e == 1).start()

    def finish(b, k, j, source, target):
        rows = pl.ds(k * R, R)
        acc[...] = part[b, k, j, rows_at(me), :].astype(jnp.float32)

        @pl.when(me > 0)
        def _():
            rs(b, 0, k, j, me, True).wait_recv()
            acc[...] += rbuf[b, 0, k, j, rows_at(me), :].astype(jnp.float32)

        @pl.when(me < n - 1)
        def _():
            rs(b, 1, k, j, me, True).wait_recv()
            acc[...] += rbuf[b, 1, k, j, rows_at(me), :].astype(jnp.float32)

        target[rows, cols_at(j)] = (
            source[rows, cols_at(j)].astype(jnp.float32) + 0.5 * acc[...]
        ).astype(jnp.bfloat16)

    def gathered(b):
        for way in range(2):
            for i in range(1, n):
                @pl.when(me == (i - 1 if way == 0 else n - i))
                def _():
                    where = xg.at[b, :, pl.ds(0, i * R), :]
                    remote(where, where, ag_s.at[b, way], ag_s.at[b, way], {"fs": mate}).wait_send()

    def ship_done(b):
        where = part.at[b, :, :, pl.ds(0, (n - 1) * R), :]
        remote(where, where, rs_s.at[b], rs_s.at[b], {"fs": mate}).wait_send()

    for u in range(PIECES[0]):
        y_send(u)
    for b in range(2):
        gain_load(b).wait()
    for k in range(K):
        load(k).wait()
        normalize(0, k, stream)
    for u in range(PIECES[0], HELD):
        y_send(u)

    for kind, args in plan(n, J, K):
        with jax.named_scope(kind + "_" + "_".join(map(str, args))):
            if kind == "y":
                y_event(*args)
                if args[0] == RESUME:
                    for u in range(HELD, U):
                        y_send(u)
            elif kind == "x":
                x_event(*args)
            elif kind == "c":
                complete(*args)
            elif kind == "o":
                nearby(*args)
            elif kind == "a":
                ag_step(*args)
            elif kind == "h":
                hidden_of(*args)
            elif kind == "p":
                partial_of(*args)
            elif kind == "r":
                hop(*args)
            elif kind == "f":
                finish(*args, *((stream, mid) if args[0] == 0 else (mid, out)))
            elif kind == "n":
                normalize(*args, mid)
            elif kind == "d":
                sent()
            elif kind == "g":
                gathered(*args)
            elif kind == "t":
                ship_done(*args)
            elif kind == "l":
                local_copy(*args).start()
                c_copy(*args).start()

    ship_done(1)


def plan(n, J, K, tune=TUNE):
    items = []

    def at(time, kind, *args):
        items.append((time, len(items), kind, args))

    b0, slots, lag, ends, hops, late, own, early = tune
    whole = J * K
    ready = []
    came = 0
    for u, (a, p) in enumerate(UNITS):
        tau = whole / PIECES[a]
        came += tau
        delay = early if a < 2 else late
        at(came + 0.8, "y", u)
        at(came + tau + delay, "x", u)
        if p == PIECES[a] - 1:
            ready.append(came + tau + delay + 0.1)
    for s in range(1, n):
        for k in range(K):
            at(whole * (s - 1) + J * (k + 1) + 0.9, "a", 0, k, s)
    for a in range(6):
        at(ready[a + 1 if a % 3 == 0 else a], "c", a)
        at(a * own, "l", a)
        at(ready[1] if a < 3 else ready[4], "o", a)
    arrived = [whole * (n - 2) + J * (k + 1) + 1.0 for k in range(K)]
    for b in range(2):
        first = min(3, K) if b == 0 else min(2, K)
        order = [(k, 0) for k in range(first)] + [(k, j) for k in range(first) for j in range(1, J)]
        order += [(k, j) for k in range(first, K) for j in range(J)]
        begun = set()
        done = [0] * K
        now = ready[1] + b0 if b == 0 else max(now, ready[4])
        for place, (k, j) in enumerate(order):
            now = max(now, arrived[k], ready[3 * b + 2] if j > 0 else 0)
            if k not in begun:
                begun.add(k)
                at(now + 0.01, "h", b, k)
            at(now + 0.02, "p", b, k, j)
            spread = b == 1 and k == K - 1
            for q in range(n - 1):
                for e in range(1, n - q):
                    wide = (n - 1 - q - e) / (n - 1)
                    if spread:
                        wide = wide * J + 0.03
                    at(now + 0.03 + lag[b] * q + wide * slots[b], "r", b, k, j, q, e)
            end = now + ends[b] + (0.01 * j if not spread else J * 0.5)
            at(end, "f", b, k, j)
            done[k] = max(done[k], end)
            now += slots[b]
        for k in range(K):
            if b == 0:
                at(done[k] + 0.03, "n", 1, k)
                for s in range(1, n):
                    at(done[k] + 0.04 + hops[k // ((K + 1) // 2)] * s, "a", 1, k, s)
                arrived[k] = done[k] + 0.05 + hops[k // ((K + 1) // 2)] * (n - 1)
            else:
                at(done[k] + 0.03, "s", k)
    at(now - slots[1], "d")
    for b in range(2):
        at(now - slots[1] * (2 - b), "g", b)
    at(now - slots[1], "t", 0)
    if (n, J, K) == ORDER_FOR:
        return [items[i][2:] for i in ORDER]
    items.sort(key=lambda item: item[:2])
    return [item[2:] for item in items]


def local(sizes_of_mesh, stream, gain_a, gate_a, up_a, down_a, gain_b, gate_b, up_b, down_b):
    G, m, n = sizes_of_mesh
    T, D = stream.shape
    F = gate_a.shape[1]
    Y = m // CORES
    J = Y if Y <= 2 else 1
    K = BATCHES
    U = len(UNITS)
    bf16 = jnp.bfloat16
    anywhere = pl.BlockSpec(memory_space=pl.ANY)
    dma = pltpu.SemaphoreType.DMA
    return pl.pallas_call(
        functools.partial(kernel, (G, m, n, T, D, F, J, K)),
        out_shape=pltpu.VMEM((T, D), bf16),
        in_specs=[anywhere] * 9,
        out_specs=pl.BlockSpec(memory_space=pltpu.VMEM),
        scratch_shapes=[
            pltpu.VMEM((2, 2, D, F), bf16),
            pltpu.VMEM((2, F, D), bf16),
            pltpu.VMEM((2, K, n * T // K, D), bf16),
            pltpu.VMEM((K, n * T // K, F), bf16),
            pltpu.VMEM((2, K, J, n * T // K, D // J), bf16),
            pltpu.VMEM((2, 2, K, J, n * T // K, D // J), bf16),
            pltpu.VMEM((T // K, D // J), jnp.float32),
            pltpu.VMEM((T, D), bf16),
            pltpu.VMEM((T, D), bf16),
            pltpu.VMEM((D,), bf16),
            pltpu.VMEM((D,), bf16),
            dma((K + 2,)),
            dma(()), dma((U, Y - 1)),
            dma(()), dma((U, Y - 1, G - 1)),
            dma(()), dma((6,)),
            dma(()), dma((6,)),
            dma((6,)),
            dma((2, 2)), dma((K, n)),
            dma((2,)), dma((K, J, n + 1)),
        ],
        compiler_params=pltpu.CompilerParams(
            collective_id=0, has_side_effects=True, vmem_limit_bytes=VMEM_LIMIT
        ),
    )(
        stream, gain_a, gain_b,
        gate_a, up_a, down_a, gate_b, up_b, down_b,
    )


def solution(mesh):
    shape = mesh.shape
    in_specs = (
        P(("grp", "fs", "tp"), None),
        P(),
        P("fs", "tp"),
        P("fs", "tp"),
        P("tp", "fs"),
        P(),
        P("fs", "tp"),
        P("fs", "tp"),
        P("tp", "fs"),
    )
    out_specs = P(("grp", "fs", "tp"), None)
    body = functools.partial(local, (shape["grp"], shape["fs"], shape["tp"]))
    return jax.shard_map(body, mesh=mesh, in_specs=in_specs, out_specs=out_specs, check_vma=False)
```

```python
import functools

import jax
import jax.numpy as jnp
from jax import lax
from jax.experimental import pallas as pl
from jax.experimental.pallas import tpu as pltpu
from jax.sharding import PartitionSpec as P

MESH = pl.DeviceIdType.MESH
CORES = 2
PIECES = (8, 8, 8, 4, 4, 4)
UNITS = [(a, p) for a in range(6) for p in range(PIECES[a])]
DIRECT = (sum(PIECES[:2]) - 1,)
HELD = sum(PIECES[:2])
RESUME = HELD - 2
BATCHES = 4
ORDER_FOR = (4, 2, 4)
ORDER = (
    85, 0, 2, 88, 4, 72, 1, 6, 91, 3, 8, 73, 5, 10, 94, 7, 12, 74, 9, 14,
    97, 11, 16, 75, 13, 18, 100, 15, 20, 76, 17, 22, 19, 24, 77, 21, 26, 23, 28, 78,
    25, 30, 27, 79, 31, 86, 89, 92, 32, 29, 80, 84, 87, 102, 34, 95, 103, 106, 81, 36,
    111, 101, 112, 105, 104, 82, 38, 40, 120, 121, 42, 108, 115, 39, 44, 123, 124, 83, 46, 37,
    41, 107, 153, 113, 48, 117, 35, 33, 122, 109, 114, 154, 125, 126, 47, 43, 45, 90, 50, 129,
    132, 131, 110, 118, 137, 145, 162, 127, 98, 140, 134, 52, 133, 130, 54, 142, 116, 148, 146, 128,
    135, 139, 56, 136, 150, 170, 143, 119, 55, 141, 147, 138, 255, 53, 58, 60, 157, 151, 171, 149,
    165, 62, 51, 57, 144, 174, 172, 49, 159, 163, 152, 167, 64, 66, 178, 164, 175, 61, 63, 59,
    93, 68, 173, 96, 186, 156, 168, 187, 188, 190, 160, 70, 166, 158, 176, 155, 189, 69, 65, 179,
    169, 161, 182, 67, 71, 99, 204, 192, 177, 206, 207, 195, 212, 196, 191, 215, 198, 199, 214, 180,
    205, 213, 181, 197, 220, 183, 209, 257, 221, 201, 184, 224, 200, 193, 216, 223, 229, 185, 208, 232,
    202, 237, 194, 246, 210, 217, 249, 238, 241, 248, 226, 203, 240, 225, 231, 234, 211, 218, 251, 247,
    219, 243, 235, 239, 250, 252, 254, 230, 227, 242, 256, 222, 244, 233, 253, 245, 236, 228,
)
TUNE = (0.0, (3.35, 4.32), (3.02, 5.12), (7.18, 13.38), (2.82, 6.01), 4.7, 2.0, 2.9)
VMEM_LIMIT = 60 * 1024 * 1024


def kernel(
    sizes,
    stream_hbm, gain_a, gain_b, gate_a, up_a, down_a, gate_b, up_b, down_b,
    out,
    gu, dn, xg, hid, part, rbuf, acc, mid, stream, scale_a, scale_b,
    i_s, y_s, y_r, x_s, x_r, c_s, c_r, f_s, f_r, l_s, ag_s, ag_r, rs_s, rs_r,
):
    G, m, n, T, D, F, J, K = sizes
    Y = m // CORES
    C = D // J
    R = T // K
    U = len(UNITS)
    gains = (scale_a, scale_b)
    weights = (gate_a, up_a, down_a, gate_b, up_b, down_b)
    g = lax.axis_index("grp")
    fs = lax.axis_index("fs")
    me = lax.axis_index("tp")
    y = fs // CORES
    c = lax.rem(fs, CORES)
    mate = y * CORES + (CORES - 1 - c)
    right = lax.rem(me + 1, n)
    left = lax.rem(me + n - 1, n)

    def row_of(k):
        return lax.rem(y + k + Y, Y) * CORES + c

    def grp_of(i):
        return lax.rem(g + i + G, G)

    def load(k):
        rows = pl.ds(k * R, R)
        return pltpu.make_async_copy(stream_hbm.at[rows, :], stream.at[rows, :], i_s.at[k])

    def gain_load(b):
        return pltpu.make_async_copy((gain_a, gain_b)[b], gains[b], i_s.at[K + b])

    barrier = pltpu.get_barrier_semaphore()
    for k in range(1, Y):
        pl.semaphore_signal(barrier, inc=1, device_id={"fs": row_of(k)}, device_id_type=MESH)
    for i in range(1, G):
        pl.semaphore_signal(barrier, inc=1, device_id={"grp": grp_of(i)}, device_id_type=MESH)
    pl.semaphore_signal(barrier, inc=1, device_id={"fs": mate}, device_id_type=MESH)

    @pl.when(me < n - 1)
    def _():
        pl.semaphore_signal(barrier, inc=1, device_id={"tp": right}, device_id_type=MESH)

    @pl.when(me > 0)
    def _():
        pl.semaphore_signal(barrier, inc=1, device_id={"tp": left}, device_id_type=MESH)

    for k in range(K):
        load(k).start()
    for b in range(2):
        gain_load(b).start()

    @pl.when(jnp.logical_and(me > 0, me < n - 1))
    def _():
        pl.semaphore_wait(barrier, Y - 1 + G - 1 + 1 + 2)

    @pl.when(jnp.logical_not(jnp.logical_and(me > 0, me < n - 1)))
    def _():
        pl.semaphore_wait(barrier, Y - 1 + G - 1 + 1 + 1)

    def rows_of(a):
        return weights[a].shape[0]

    def piece_rows(u, h):
        a, p = UNITS[u]
        rows = rows_of(a) // G
        sub = rows // PIECES[a]
        return pl.multiple_of(h * rows + p * sub, sub), sub

    def own(u, h):
        off, sub = piece_rows(u, h)
        return weights[UNITS[u][0]].at[pl.ds(off, sub), :]

    def place(a, j, off, count):
        b, t = a // 3, a % 3
        if t < 2:
            return gu.at[b, t, pl.ds(pl.multiple_of(j * rows_of(a) + off, count), count), :]
        cols = D // m
        return dn.at[b, pl.ds(off, count), pl.ds(pl.multiple_of(j * cols, cols), cols)]

    def slot(u, j, h):
        off, sub = piece_rows(u, h)
        return place(UNITS[u][0], j, off, sub)

    def whole(a, j):
        return place(a, j, 0, rows_of(a))

    def remote(src, dst, ss, rs, dev):
        return pltpu.make_async_remote_copy(
            src_ref=src, dst_ref=dst, send_sem=ss, recv_sem=rs, device_id=dev, device_id_type=MESH
        )

    def local_copy(a):
        return pltpu.make_async_copy(weights[a], whole(a, fs), l_s.at[a])

    def y_copy(a, k):
        return remote(own(a, g), slot(a, fs, g), y_s, y_r.at[a, k - 1], {"fs": row_of(k)})

    def y_arrived(a, k):
        remote(own(a, g), slot(a, row_of(-k), g), y_s, y_r.at[a, k - 1], {"fs": row_of(k)}).wait_recv()

    def c_copy(a):
        return remote(weights[a], whole(a, fs), c_s, c_r.at[a], {"fs": mate})

    def c_arrived(a):
        remote(weights[a], whole(a, mate), c_s, c_r.at[a], {"fs": mate}).wait_recv()

    def x_copy(a, k, i):
        where = slot(a, row_of(-k), g)
        return remote(where, where, x_s, x_r.at[a, k - 1, i - 1], {"grp": grp_of(i)})

    def x_arrived(a, k, i):
        where = slot(a, row_of(-k), grp_of(-i))
        remote(where, where, x_s, x_r.at[a, k - 1, i - 1], {"grp": grp_of(i)}).wait_recv()

    def f_copy(a, k, i):
        where = slot(a, row_of(-k), grp_of(-i))
        return remote(where, where, f_s, f_r.at[UNITS[a][0]], {"fs": mate})

    def y_send(a):
        for k in range(1, Y):
            y_copy(a, k).start()
            for i in range(1, G):
                if a in DIRECT:
                    h = grp_of(-i)
                    remote(
                        own(a, h), slot(a, fs, h), x_s, x_r.at[a, k - 1, i - 1], {"fs": row_of(k)}
                    ).start()

    def y_event(a):
        for k in range(1, Y):
            y_arrived(a, k)
            for i in range(1, G):
                if a not in DIRECT:
                    x_copy(a, k, i).start()
            f_copy(a, k, 0).start()

    def x_event(a):
        for k in range(1, Y):
            for i in range(1, G):
                x_arrived(a, k, i)
                f_copy(a, k, i).start()

    def nearby(a):
        local_copy(a).wait()
        c_arrived(a)

    far = (Y - 1) * (D // m)

    def complete(a):
        where = gu.at[0, 0, pl.ds(0, far), :]
        remote(where, where, f_s, f_r.at[a], {"fs": mate}).wait_recv()

    def sent():
        for rows, sem in (
            (D // m, c_s), (far // G, y_s), (far // G * (G - 1), x_s), (far, f_s),
        ):
            where = gu.at[:, :, pl.ds(0, 6 * rows // 4), :]
            remote(where, where, sem, f_r.at[0], {"fs": mate}).wait_send()

    def rows_at(blk):
        return pl.ds(pl.multiple_of(blk * R, R), R)

    def cols_at(j):
        return pl.ds(pl.multiple_of(lax.rem(y + j, J) * C, C), C)

    def ag(b, way, k, blk):
        where = xg.at[b, k, rows_at(blk), :]
        return remote(where, where, ag_s.at[b, way], ag_r.at[k, blk], {"tp": right if way == 0 else left})

    def ag_step(b, k, s):
        for way in range(2):
            blk = me - s if way == 0 else me + s

            @pl.when(blk >= 0 if way == 0 else blk < n)
            def _():
                ag(b, way, k, blk).wait_recv()

                @pl.when(me < n - 1 if way == 0 else me > 0)
                def _():
                    ag(b, way, k, blk).start()

    def normalize(b, k, source):
        rows = pl.ds(k * R, R)
        v = source[rows, :].astype(jnp.float32)
        scale = lax.rsqrt(jnp.mean(v * v, axis=-1, keepdims=True) + 1e-06)
        xg[b, k, rows_at(me), :] = (v * scale * gains[b][...].astype(jnp.float32).reshape(1, D)).astype(jnp.bfloat16)

        @pl.when(me < n - 1)
        def _():
            ag(b, 0, k, me).start()

        @pl.when(me > 0)
        def _():
            ag(b, 1, k, me).start()

    def hidden_of(b, k):
        tile = min(512, F)

        @pl.loop(0, F // tile)
        def _(q):
            cols = pl.ds(pl.multiple_of(q * tile, tile), tile)
            x = xg[b, k]
            gate = jnp.dot(x, gu[b, 0, :, cols], preferred_element_type=jnp.float32)
            up = jnp.dot(x, gu[b, 1, :, cols], preferred_element_type=jnp.float32)
            hid[k, :, cols] = (gate / (1.0 + jnp.exp(-gate)) * up).astype(jnp.bfloat16)

    def rs(b, way, k, j, d, last=False):
        arrived = rs_r.at[k, j, n if last and way == 1 else d]
        return remote(
            part.at[b, k, j, rows_at(d), :], rbuf.at[b, way, k, j, rows_at(d), :],
            rs_s.at[b], arrived, {"tp": right if way == 0 else left},
        )

    def partial_of(b, k, j):
        tile = min(512, C)

        @pl.loop(0, C // tile)
        def _(q):
            cols = pl.ds(pl.multiple_of(lax.rem(y + j, J) * C + q * tile, tile), tile)
            dst = pl.ds(pl.multiple_of(q * tile, tile), tile)
            part[b, k, j, :, dst] = jnp.dot(
                hid[k], dn[b, :, cols], preferred_element_type=jnp.float32
            ).astype(jnp.bfloat16)

    def hop(b, k, j, q, e):
        for way in range(2):
            @pl.when(me == (q if way == 0 else n - 1 - q))
            def _():
                d = q + e if way == 0 else n - 1 - q - e
                if q > 0:
                    rs(b, way, k, j, d).wait_recv()
                    part[b, k, j, rows_at(d), :] = (
                        part[b, k, j, rows_at(d), :].astype(jnp.float32)
                        + rbuf[b, way, k, j, rows_at(d), :].astype(jnp.float32)
                    ).astype(jnp.bfloat16)
                rs(b, way, k, j, d, e == 1).start()

    def finish(b, k, j, source, target):
        rows = pl.ds(k * R, R)
        acc[...] = part[b, k, j, rows_at(me), :].astype(jnp.float32)

        @pl.when(me > 0)
        def _():
            rs(b, 0, k, j, me, True).wait_recv()
            acc[...] += rbuf[b, 0, k, j, rows_at(me), :].astype(jnp.float32)

        @pl.when(me < n - 1)
        def _():
            rs(b, 1, k, j, me, True).wait_recv()
            acc[...] += rbuf[b, 1, k, j, rows_at(me), :].astype(jnp.float32)

        target[rows, cols_at(j)] = (
            source[rows, cols_at(j)].astype(jnp.float32) + 0.5 * acc[...]
        ).astype(jnp.bfloat16)

    def gathered(b):
        for way in range(2):
            for i in range(1, n):
                @pl.when(me == (i - 1 if way == 0 else n - i))
                def _():
                    where = xg.at[b, :, pl.ds(0, i * R), :]
                    remote(where, where, ag_s.at[b, way], ag_s.at[b, way], {"fs": mate}).wait_send()

    def ship_done(b):
        where = part.at[b, :, :, pl.ds(0, (n - 1) * R), :]
        remote(where, where, rs_s.at[b], rs_s.at[b], {"fs": mate}).wait_send()

    for u in range(PIECES[0]):
        y_send(u)
    for b in range(2):
        gain_load(b).wait()
    for k in range(K):
        load(k).wait()
        normalize(0, k, stream)
    for u in range(PIECES[0], HELD):
        y_send(u)

    for kind, args in plan(n, J, K):
        with jax.named_scope(kind + "_" + "_".join(map(str, args))):
            if kind == "y":
                y_event(*args)
                if args[0] == RESUME:
                    for u in range(HELD, U):
                        y_send(u)
            elif kind == "x":
                x_event(*args)
            elif kind == "c":
                complete(*args)
            elif kind == "o":
                nearby(*args)
            elif kind == "a":
                ag_step(*args)
            elif kind == "h":
                hidden_of(*args)
            elif kind == "p":
                partial_of(*args)
            elif kind == "r":
                hop(*args)
            elif kind == "f":
                finish(*args, *((stream, mid) if args[0] == 0 else (mid, out)))
            elif kind == "n":
                normalize(*args, mid)
            elif kind == "d":
                sent()
            elif kind == "g":
                gathered(*args)
            elif kind == "t":
                ship_done(*args)
            elif kind == "l":
                local_copy(*args).start()
                c_copy(*args).start()

    ship_done(1)


def plan(n, J, K, tune=TUNE):
    items = []

    def at(time, kind, *args):
        items.append((time, len(items), kind, args))

    b0, slots, lag, ends, hops, late, own, early = tune
    whole = J * K
    ready = []
    came = 0
    for u, (a, p) in enumerate(UNITS):
        tau = whole / PIECES[a]
        came += tau
        delay = early if a < 2 else late
        at(came + 0.8, "y", u)
        at(came + tau + delay, "x", u)
        if p == PIECES[a] - 1:
            ready.append(came + tau + delay + 0.1)
    for s in range(1, n):
        for k in range(K):
            at(whole * (s - 1) + J * (k + 1) + 0.9, "a", 0, k, s)
    for a in range(6):
        at(ready[a + 1 if a % 3 == 0 else a], "c", a)
        at(a * own, "l", a)
        at(ready[1] if a < 3 else ready[4], "o", a)
    arrived = [whole * (n - 2) + J * (k + 1) + 1.0 for k in range(K)]
    for b in range(2):
        first = min(3, K) if b == 0 else min(2, K)
        order = [(k, 0) for k in range(first)] + [(k, j) for k in range(first) for j in range(1, J)]
        order += [(k, j) for k in range(first, K) for j in range(J)]
        begun = set()
        done = [0] * K
        now = ready[1] + b0 if b == 0 else max(now, ready[4])
        for place, (k, j) in enumerate(order):
            now = max(now, arrived[k], ready[3 * b + 2] if j > 0 else 0)
            if k not in begun:
                begun.add(k)
                at(now + 0.01, "h", b, k)
            at(now + 0.02, "p", b, k, j)
            spread = b == 1 and k == K - 1
            for q in range(n - 1):
                for e in range(1, n - q):
                    wide = (n - 1 - q - e) / (n - 1)
                    if spread:
                        wide = wide * J + 0.03
                    at(now + 0.03 + lag[b] * q + wide * slots[b], "r", b, k, j, q, e)
            end = now + max(ends[b], lag[b] * (n - 2) + 0.2, slots[b] * J + 0.2) + (0.01 * j if not spread else J * 0.5)
            at(end, "f", b, k, j)
            done[k] = max(done[k], end)
            now += slots[b]
        for k in range(K):
            if b == 0:
                at(done[k] + 0.03, "n", 1, k)
                for s in range(1, n):
                    at(done[k] + 0.04 + hops[k // ((K + 1) // 2)] * s, "a", 1, k, s)
                arrived[k] = done[k] + 0.05 + hops[k // ((K + 1) // 2)] * (n - 1)
    at(now - slots[1], "d")
    for b in range(2):
        at(now - slots[1] * (2 - b), "g", b)
    at(now - slots[1], "t", 0)
    if (n, J, K) == ORDER_FOR:
        return [items[i][2:] for i in ORDER]
    items.sort(key=lambda item: item[:2])
    return [item[2:] for item in items]


def local(sizes_of_mesh, stream, gain_a, gate_a, up_a, down_a, gain_b, gate_b, up_b, down_b):
    G, m, n = sizes_of_mesh
    T, D = stream.shape
    F = gate_a.shape[1]
    Y = m // CORES
    J = Y if Y <= 2 else 1
    K = BATCHES
    U = len(UNITS)
    bf16 = jnp.bfloat16
    anywhere = pl.BlockSpec(memory_space=pl.ANY)
    dma = pltpu.SemaphoreType.DMA
    return pl.pallas_call(
        functools.partial(kernel, (G, m, n, T, D, F, J, K)),
        out_shape=pltpu.VMEM((T, D), bf16),
        in_specs=[anywhere] * 9,
        out_specs=pl.BlockSpec(memory_space=pltpu.VMEM),
        scratch_shapes=[
            pltpu.VMEM((2, 2, D, F), bf16),
            pltpu.VMEM((2, F, D), bf16),
            pltpu.VMEM((2, K, n * T // K, D), bf16),
            pltpu.VMEM((K, n * T // K, F), bf16),
            pltpu.VMEM((2, K, J, n * T // K, D // J), bf16),
            pltpu.VMEM((2, 2, K, J, n * T // K, D // J), bf16),
            pltpu.VMEM((T // K, D // J), jnp.float32),
            pltpu.VMEM((T, D), bf16),
            pltpu.VMEM((T, D), bf16),
            pltpu.VMEM((D,), bf16),
            pltpu.VMEM((D,), bf16),
            dma((K + 2,)),
            dma(()), dma((U, Y - 1)),
            dma(()), dma((U, Y - 1, G - 1)),
            dma(()), dma((6,)),
            dma(()), dma((6,)),
            dma((6,)),
            dma((2, 2)), dma((K, n)),
            dma((2,)), dma((K, J, n + 1)),
        ],
        compiler_params=pltpu.CompilerParams(
            collective_id=0, has_side_effects=True, vmem_limit_bytes=VMEM_LIMIT
        ),
    )(
        stream, gain_a, gain_b,
        gate_a, up_a, down_a, gate_b, up_b, down_b,
    )


def solution(mesh):
    shape = mesh.shape
    in_specs = (
        P(("grp", "fs", "tp"), None),
        P(),
        P("fs", "tp"),
        P("fs", "tp"),
        P("tp", "fs"),
        P(),
        P("fs", "tp"),
        P("fs", "tp"),
        P("tp", "fs"),
    )
    out_specs = P(("grp", "fs", "tp"), None)
    body = functools.partial(local, (shape["grp"], shape["fs"], shape["tp"]))
    return jax.shard_map(body, mesh=mesh, in_specs=in_specs, out_specs=out_specs, check_vma=False)
```
